32 devices in a mesh: sp: 8 (over z, core), tp: 4 (over y, x).
Axes of the slice: x: 2, y: 2, z: 4, core: 2. Of those that a mesh axis runs over, the one named last changes fastest.
Arguments:
- query_heads: bfloat16 [2048, 1024], P('sp', 'tp'), may hold values from -6 to 6
- key_heads: bfloat16 [2048, 256], P('sp'), may hold values from -6 to 6
- value_heads: bfloat16 [2048, 256], P('sp'), may hold values from -24 to 24
- q_gain: float32 [64], replicated, may hold values from 0.6 to 4.5
- k_gain: float32 [64], replicated, may hold values from 0.6 to 4.5
- out_weight: bfloat16 [1024, 2048], P('tp'), may hold values from -0.1875 to 0.1875
- residual: bfloat16 [2048, 2048], P('sp', 'tp'), may hold values from -3 to 3
- norm_gain: float32 [2048], P('tp'), may hold values from 0.1 to 1.9
- routes: int32 [2048, 2], P('sp'), may hold values from 0 to 7, all different within a row; in each aligned block of 256 rows (0 to 255, 256 to 511, ...) at most 81 rows name the same one
- route_weights: float32 [2048, 2], P('sp'), may hold values from 0.5 to 1.5
- w_gate: bfloat16 [8, 2048, 4096], P('sp', None, 'tp'), may hold values from -0.125 to 0.125
- w_up: bfloat16 [8, 2048, 4096], P('sp', None, 'tp'), may hold values from -0.125 to 0.125
- w_down: bfloat16 [8, 4096, 2048], P('sp', 'tp'), may hold values from -0.1875 to 0.1875
Outputs:
- layer_out: bfloat16 [2048, 2048], P('sp', 'tp')
The draws below stay inside these ranges and needn't reach their ends.
Inputs may be any that keep to these rules, and one draw needn't show every extreme that they name: `routes`: each row names 2 different experts. Among the 256 rows of one index of sp, no expert is named more than 81 times, a bound that some block reaches.
All inputs are finite; a program needn't handle non-finite values.
Results may differ from the reference program's by a relative error of at most 0.02.
The reference program's roundings to bfloat16 on the way count: a program that leaves them out, or rounds other values in their place, can miss the bound.
Values may be sent and summed in bfloat16 or wider, within the bound.
No kernel may reach another device: no remote copies, remote signals or barrier semaphores. Data moves between devices by JAX's collectives and lax.ppermute only.
A program may use at most 64 MiB of HBM per device.

```python
import math
import jax
import jax.numpy as jnp
import numpy as np
from jax import lax

D = 2048
HQ = 16
KV = 4
E = 64
FF = 4096
TOPK = 2
GRID_W = 64
TOK_SP = 256
TOKENS = 2048
EXPERTS = 8
CAP = 81
N_SP = 8
N_TP = 4


def base_keys(key):
    drawn = jax.random.normal(jax.random.fold_in(key, 11), (TOKENS, KV * E), jnp.float32)
    return jnp.clip(drawn, -6.0, 6.0)


def draw_key_heads(key, part):
    return base_keys(key).astype(jnp.bfloat16)


def draw_query_heads(key, part):
    fresh = jax.random.normal(jax.random.fold_in(key, 23), (TOKENS, KV, HQ // KV, E), jnp.float32)
    fresh = jnp.clip(fresh, -6.0, 6.0)
    return fresh.reshape(TOKENS, HQ * E).astype(jnp.bfloat16)


def gain_of(key, salt):
    return 1.0 + 0.18 * jax.random.uniform(jax.random.fold_in(key, salt), (E,), jnp.float32, -2.0, 2.0)


def draw_q_gain(key, part):
    return gain_of(key, 31)


def draw_k_gain(key, part):
    return gain_of(key, 37)


def draw_residual(key, part):
    noise_key = jax.random.fold_in(key, 41)
    row_key = jax.random.fold_in(key, 43)
    column_pos = jnp.arange(D, dtype=jnp.float32) / D
    row_scale = jnp.exp(jax.random.uniform(row_key, (TOKENS, 1), jnp.float32, 0.0, jnp.log(2.0)))
    base = jax.random.normal(noise_key, (TOKENS, D), jnp.float32)
    column_scale = 0.05 * jnp.exp(jnp.log(10.0) * column_pos)
    values = base * row_scale * column_scale[None, :]
    return jnp.clip(values, -3.0, 3.0).astype(jnp.bfloat16)


def steps_of(rng, dims, shards, smallest, top_value):
    level = 1.0
    for axis_at, shards_of in shards:
        steps = jax.random.uniform(jax.random.fold_in(jax.random.fold_in(rng, 6), axis_at), (shards_of,), jnp.float32, smallest / len(shards), top_value / len(shards))
        level = level * jnp.repeat(jnp.exp(steps), dims[axis_at] // shards_of).reshape((-1,) + (1,) * (len(dims) - 1 - axis_at))
    return level


def deal_out(key, own, number, rows, count, top, most, slope):
    order = jax.random.permutation(key, count)
    crowded, common = load_shares(count, rows * top, most, slope, True), load_shares(count, rows * top, most, slope, False)
    places = jnp.arange(count)

    def named(tallies, turn):
        used = int((tallies > 0).sum())
        fixed = max(1, used // 4)
        shifted = fixed + (places - fixed + turn * (used - fixed)) % max(1, count - fixed)
        return jnp.zeros((count,), jnp.int32).at[order[jnp.where(places < fixed, places, shifted)]].set(jnp.asarray(tallies, jnp.int32))

    tallies = jnp.where(number % 4 == 0, named(crowded, number // 4), named(common, number - number // 4 - 1))
    mixed = jax.random.permutation(jax.random.fold_in(own, 3), count)
    giver, receiver = mixed[0:count // 2 * 2:2], mixed[1:count // 2 * 2:2]
    room = jnp.minimum(tallies[giver] - 1, most - tallies[receiver]) // 2
    room = jnp.where((giver == order[0]) | (receiver == order[0]) | (tallies[receiver] == 0), 0, jnp.maximum(room, 0))
    shifted = jax.random.randint(jax.random.fold_in(own, 4), (count // 2,), 0, 1 << 20) % (room + 1)
    tallies = tallies.at[giver].add(-shifted).at[receiver].add(shifted)
    labels = jnp.searchsorted(jnp.cumsum(tallies), jnp.arange(rows * top), side="right").astype(jnp.int32)
    table = labels.reshape(top, rows).T
    table = table[jax.random.permutation(jax.random.fold_in(own, 1), rows)]
    turn = jax.random.randint(jax.random.fold_in(own, 2), (rows, 1), 0, top)
    return jnp.take_along_axis(table, (jnp.arange(top)[None, :] + turn) % top, axis=1)


def load_shares(amount, total, bound, lean, full):
    portions = [(1 << 20) // math.isqrt(rank ** lean) + 1 for rank in range(1, amount + 1)]
    largest = bound if full else min(bound, max(-(-total // amount), total * portions[0] // sum(portions)))
    least = 1 if total - largest >= amount - 1 else 0
    holding, spare = [largest] + [least] * (amount - 1), total - largest - least * (amount - 1)
    while spare > 0:
        movable = [i for i in range(1, amount) if holding[i] < largest] or [i for i in range(1, amount) if holding[i] < bound]
        mass, remaining = sum([portions[i] for i in movable]), spare
        for i in movable:
            addition = min(bound - holding[i], max(1, remaining * portions[i] // mass), spare)
            holding[i] = holding[i] + addition
            spare = spare - addition
    return np.array(holding)


def normal_values(stream_key, dims, scale, bound, cuts=(), kind=jnp.bfloat16):
    level = steps_of(stream_key, dims, cuts, -0.22, 0.18) if cuts else 1.0
    array = jax.random.normal(stream_key, dims, jnp.float32) * scale * level
    return jnp.minimum(jnp.maximum(array, -bound), bound).astype(kind)


def setup_inputs(seed: int = 0) -> dict:
    arg_keys = jax.random.split(jax.random.key(seed), 14)
    query_heads = draw_query_heads(jax.random.fold_in(arg_keys[13], 71), 0)
    key_heads = draw_key_heads(jax.random.fold_in(arg_keys[13], 71), 0)
    value_heads = normal_values(arg_keys[2], (TOKENS, KV * E), 4.0, 24.0, ((0, 8),))
    q_gain = draw_q_gain(jax.random.fold_in(arg_keys[13], 71), 0)
    k_gain = draw_k_gain(jax.random.fold_in(arg_keys[13], 71), 0)
    out_weight = normal_values(arg_keys[5], (HQ * E, D), (HQ * E) ** -0.5, 0.1875, ((0, 4),))
    residual = draw_residual(jax.random.fold_in(arg_keys[13], 71), 0)
    norm_gain = jnp.clip(1.0 + 0.18 * jax.random.normal(arg_keys[7], (D,), jnp.float32), 0.1, 1.9)
    routes_keys = jax.random.split(jax.random.fold_in(arg_keys[8], 1), TOKENS // TOK_SP)
    routes_turns = jax.random.permutation(jax.random.fold_in(arg_keys[8], 3), TOKENS // TOK_SP)
    routes = jax.vmap(lambda own, number: deal_out(jax.random.fold_in(arg_keys[8], 2), own, number, TOK_SP, EXPERTS, TOPK, CAP, 1))(routes_keys, routes_turns).reshape((TOKENS, TOPK))
    route_weights = jnp.clip(0.5 + 1.0 * jax.random.uniform(arg_keys[9], (TOKENS, TOPK), jnp.float32) ** steps_of(arg_keys[9], (TOKENS, TOPK), ((0, 8),), -0.2, 0.2), 0.5, 1.5)
    w_gate = normal_values(arg_keys[10], (EXPERTS, D, FF), D ** -0.5, 0.125, ((0, 8), (2, 4)))
    w_up = normal_values(arg_keys[11], (EXPERTS, D, FF), D ** -0.5, 0.125, ((0, 8), (2, 4)))
    w_down = normal_values(arg_keys[12], (EXPERTS, FF, D), (FF // 4) ** -0.5, 0.1875, ((0, 8), (1, 4)))
    return {"query_heads": query_heads, "key_heads": key_heads, "value_heads": value_heads, "q_gain": q_gain, "k_gain": k_gain, "out_weight": out_weight, "residual": residual, "norm_gain": norm_gain, "routes": routes, "route_weights": route_weights, "w_gate": w_gate, "w_up": w_up, "w_down": w_down}


norm_eps = 1e-06
rope_base = 10000.0

def normalize(values_f, gain):
    mean_sq = lax.optimization_barrier(jnp.mean(values_f * values_f, axis=-1, keepdims=True))
    return values_f * lax.rsqrt(mean_sq + norm_eps) * gain

def rotate(values_f, positions):
    head_width = values_f.shape[-1]
    half_width = head_width // 2
    quarter_width = half_width // 2
    frequency = rope_base ** (-jnp.arange(quarter_width, dtype=jnp.float32) / quarter_width)
    grid_rows = (positions // GRID_W).astype(jnp.float32)
    grid_cols = (positions % GRID_W).astype(jnp.float32)
    shape = (values_f.shape[0],) + (1,) * (values_f.ndim - 2) + (quarter_width,)
    pieces = []
    for coords, offset_lo in ((grid_rows, 0), (grid_cols, half_width)):
        angles = coords[:, None] * frequency[None, :]
        cosine = jnp.cos(angles).reshape(shape)
        sines = jnp.sin(angles).reshape(shape)
        first_part = values_f[..., offset_lo:offset_lo + quarter_width]
        second_part = values_f[..., offset_lo + quarter_width:offset_lo + half_width]
        pieces.append(first_part * cosine - second_part * sines)
        pieces.append(second_part * cosine + first_part * sines)
    return jnp.concatenate(pieces, axis=-1)

def slots_of(assign):
    onehot = (assign[:, None] == jnp.arange(EXPERTS, dtype=jnp.int32)[None, :]).astype(jnp.int32)
    before = jnp.cumsum(onehot, axis=0) - onehot
    return lax.optimization_barrier(jnp.sum(before * onehot, axis=1)).astype(jnp.int32)

def reference(query_heads, key_heads, value_heads, q_gain, k_gain, out_weight, residual, norm_gain, routes, route_weights, w_gate, w_up, w_down):
    group_size = HQ // KV
    positions = jnp.arange(TOKENS, dtype=jnp.int32)
    query_f = query_heads.astype(jnp.float32).reshape(TOKENS, KV, group_size, E)
    q_turned = rotate(normalize(query_f, q_gain), positions).astype(jnp.bfloat16)
    key_f = key_heads.astype(jnp.float32).reshape(TOKENS, KV, E)
    k_turned = rotate(normalize(key_f, k_gain), positions).astype(jnp.bfloat16).astype(jnp.float32)
    value_f = value_heads.astype(jnp.float32).reshape(TOKENS, KV, E)

    def query_block(block_q):
        scores = jnp.einsum('qcge,kce->cgqk', block_q.astype(jnp.float32), k_turned) * E ** (-0.5)
        row_max = lax.optimization_barrier(jnp.max(scores, axis=-1, keepdims=True))
        exped = jnp.exp(scores - row_max)
        denominator = lax.optimization_barrier(jnp.sum(exped, axis=-1))
        rounded = lax.optimization_barrier(exped.astype(jnp.bfloat16))
        weighted = jnp.einsum('cgqk,kce->qcge', rounded.astype(jnp.float32), value_f)
        return (weighted / jnp.transpose(denominator, (2, 0, 1))[..., None]).astype(jnp.bfloat16)
    attended = lax.map(query_block, q_turned.reshape(N_SP, TOK_SP, KV, group_size, E))
    attended = attended.reshape(TOKENS, HQ * E)
    rows_tp = HQ * E // N_TP
    head_blocks = attended.reshape(TOKENS, N_TP, rows_tp).transpose(1, 0, 2)
    weight_blocks = out_weight.reshape(N_TP, rows_tp, D)

    def add_block(running, operands):
        partial_value = jnp.dot(operands[0], operands[1], preferred_element_type=jnp.float32).astype(jnp.bfloat16)
        partial_value = lax.optimization_barrier(partial_value)
        return (running + partial_value.astype(jnp.float32), None)
    attn_out, _ = lax.scan(add_block, jnp.zeros((TOKENS, D), jnp.float32), (head_blocks, weight_blocks))
    after_attn = residual.astype(jnp.float32) + attn_out
    mean_sq = lax.optimization_barrier(jnp.mean(after_attn * after_attn, axis=1, keepdims=True))
    normed = (after_attn * lax.rsqrt(mean_sq + norm_eps) * norm_gain).astype(jnp.bfloat16)
    assign = routes.reshape(N_SP, TOK_SP * TOPK)
    slot_rank = jax.vmap(slots_of)(assign)
    slot_index = assign * CAP + slot_rank
    token_local = (jnp.arange(TOK_SP * TOPK, dtype=jnp.int32) // TOPK).astype(jnp.int32)

    def table_of(indices):
        return jnp.full((EXPERTS * CAP,), TOK_SP, jnp.int32).at[indices].set(token_local)
    slot_token = jax.vmap(table_of)(slot_index)
    group_start = (jnp.arange(N_SP, dtype=jnp.int32) * TOK_SP)[:, None]
    global_token = jnp.where(slot_token < TOK_SP, slot_token + group_start, TOKENS).astype(jnp.int32)
    row_index = global_token.reshape(N_SP, EXPERTS, CAP).transpose(1, 0, 2).reshape(EXPERTS, N_SP * CAP)
    padded = jnp.concatenate([normed, jnp.zeros((1, D), jnp.bfloat16)], axis=0)
    hidden_tp = FF // N_TP

    def expert(operands):
        indices, gate_w, up_w, down_w = operands
        gathered = padded[indices]
        gate_sum = jnp.dot(gathered, gate_w, preferred_element_type=jnp.float32)
        up_sum = jnp.dot(gathered, up_w, preferred_element_type=jnp.float32)
        activated = (jax.nn.silu(gate_sum) * up_sum).astype(jnp.bfloat16)
        act_blocks = activated.reshape(N_SP * CAP, N_TP, hidden_tp).transpose(1, 0, 2)
        down_blocks = down_w.reshape(N_TP, hidden_tp, D)

        def add_part(running, pair):
            partial_value = jnp.dot(pair[0], pair[1], preferred_element_type=jnp.float32).astype(jnp.bfloat16)
            partial_value = lax.optimization_barrier(partial_value)
            return (running + partial_value.astype(jnp.float32), None)
        total, _ = lax.scan(add_part, jnp.zeros((N_SP * CAP, D), jnp.float32), (act_blocks, down_blocks))
        return total.astype(jnp.bfloat16)
    expert_rows = lax.map(expert, (row_index, w_gate, w_up, w_down)).reshape(EXPERTS, N_SP, CAP, D)
    group_idx = jnp.arange(N_SP, dtype=jnp.int32)[:, None]
    picked = expert_rows[assign, group_idx, slot_rank].astype(jnp.float32)
    picked = picked.reshape(TOKENS, TOPK, D)
    expert_mix = lax.optimization_barrier(jnp.sum(picked * route_weights[:, :, None], axis=1))
    return (after_attn + expert_mix).astype(jnp.bfloat16)
```

```python
import jax
import jax.numpy as jnp
from jax import lax
from jax.experimental import pallas as pl
from jax.experimental.pallas import tpu as pltpu
from jax.sharding import PartitionSpec as P

D = 2048
HQ = 16
KV = 4
E = 64
TOPK = 2
GRID_W = 64
GROUPS = 4

norm_eps = 1e-06
rope_base = 10000.0
bf16 = jnp.bfloat16
f32 = jnp.float32


def turn(values, gain, heads, positions):
    rows, width = values.shape
    lane = jnp.arange(width, dtype=jnp.int32) % E
    quarter = E // 4
    same_head = (jnp.arange(width)[:, None] // E == jnp.arange(heads)[None, :]).astype(f32)
    mean_sq = jnp.dot(values * values, same_head, precision=lax.Precision.HIGHEST) / E
    scale = jnp.dot(
        lax.rsqrt(mean_sq + norm_eps), same_head.T, precision=lax.Precision.HIGHEST
    )
    normed = values * scale * jnp.tile(gain, heads)[None, :]
    frequency = rope_base ** (-jnp.arange(quarter, dtype=f32) / quarter)
    grid_rows = (positions // GRID_W).astype(f32)
    grid_cols = (positions % GRID_W).astype(f32)
    angles = jnp.concatenate(
        [grid_rows[:, None] * frequency[None, :], grid_cols[:, None] * frequency[None, :]], axis=1
    )
    cosine = jnp.cos(angles)
    sines = jnp.sin(angles)
    cos_lane = jnp.concatenate([cosine[:, :quarter]] * 2 + [cosine[:, quarter:]] * 2, axis=1)
    sin_lane = jnp.concatenate(
        [-sines[:, :quarter], sines[:, :quarter], -sines[:, quarter:], sines[:, quarter:]], axis=1
    )
    first = (lane % (2 * quarter)) < quarter
    other = jnp.where(
        first[None, :], jnp.roll(normed, -quarter, axis=1), jnp.roll(normed, quarter, axis=1)
    )
    return (
        normed * jnp.tile(cos_lane, (1, heads)) + other * jnp.tile(sin_lane, (1, heads))
    ).astype(bf16)


def write_parts(value, offs_ref, outs, blocks, width):
    for ref, indices in zip(outs, blocks):
        for place, index in enumerate(indices):
            start = offs_ref[index]
            if width < D:
                start = pl.multiple_of(start, 128)
                ref[:, place * width : (place + 1) * width] = value[:, pl.ds(start, width)].astype(
                    bf16
                )
            else:
                ref[...] = value[...].astype(bf16)


def attention_kernel(blocks, width, kv_count, per_kv, pieces):
    def body(offs_ref, q_ref, *refs):
        kv_refs = refs[:pieces]
        weight_ref = refs[pieces]
        outs = refs[pieces + 1 : pieces + 1 + len(blocks)]
        kv_all, attended, acc = refs[pieces + 1 + len(blocks) :]
        rows = kv_refs[0].shape[0]
        for n in range(pieces):
            kv_all[n * rows : (n + 1) * rows, :] = kv_refs[n][...]
        for c in range(kv_count):
            kv = kv_all[:, c * 2 * E : (c + 1) * 2 * E]
            for g in range(per_kv):
                h = c * per_kv + g
                q = q_ref[:, h * 2 * E : (h + 1) * 2 * E]
                scores = lax.dot_general(
                    q, kv, (((1,), (1,)), ((), ())), preferred_element_type=f32
                )
                scores = scores * (E**-0.5)
                exped = jnp.exp(scores - jnp.max(scores, axis=1, keepdims=True))
                total = jnp.sum(exped, axis=1, keepdims=True)
                mixed = jnp.dot(exped.astype(bf16), kv, preferred_element_type=f32)
                attended[:, h * E : (h + 1) * E] = (mixed[:, E:] / total).astype(bf16)
        acc[...] = jnp.dot(attended[...], weight_ref[...], preferred_element_type=f32)
        write_parts(acc, offs_ref, outs, blocks, width)

    return body


def expert_kernel(blocks, width, in_offs, pieces, steps):
    def body(offs_ref, gain_ref, *refs):
        u_refs = refs[:pieces]
        gate_ref, up_ref, down_ref = refs[pieces : pieces + 3]
        outs = refs[pieces + 3 : pieces + 3 + len(blocks)]
        acc, scale = refs[pieces + 3 + len(blocks) :]
        step = pl.program_id(0)

        @pl.when(step == 0)
        def _():
            total = None
            for n in range(pieces):
                wide = u_refs[n].shape[1]
                start = pl.multiple_of(offs_ref[in_offs[n]], 128)
                plain = u_refs[n][...].astype(f32) / gain_ref[:, pl.ds(start, wide)]
                part = jnp.sum(plain * plain, axis=1, keepdims=True)
                total = part if total is None else total + part
            scale[...] = jnp.broadcast_to(lax.rsqrt(total / D + norm_eps), scale.shape)

        gate = None
        up = None
        for n in range(pieces):
            wide = u_refs[n].shape[1]
            start = pl.multiple_of(offs_ref[in_offs[n]], 128)
            u = u_refs[n][...]
            g = jnp.dot(u, gate_ref[0, pl.ds(start, wide), :], preferred_element_type=f32)
            v = jnp.dot(u, up_ref[0, pl.ds(start, wide), :], preferred_element_type=f32)
            gate = g if gate is None else gate + g
            up = v if up is None else up + v
        factor = scale[:, 0:1]
        gate = gate * factor
        up = up * factor
        act = (gate / (1.0 + jnp.exp(-gate)) * up).astype(bf16)
        part = jnp.dot(act, down_ref[0], preferred_element_type=f32)

        @pl.when(step == 0)
        def _():
            acc[...] = part

        @pl.when(step > 0)
        def _():
            acc[...] += part

        @pl.when(step == steps - 1)
        def _():
            write_parts(acc, offs_ref, outs, blocks, width)

    return body


def shards(
    query_heads,
    key_heads,
    value_heads,
    q_gain,
    k_gain,
    out_weight,
    residual,
    norm_gain,
    routes,
    route_weights,
    w_gate,
    w_up,
    w_down,
):
    tok_rows = query_heads.shape[0]
    head_local = query_heads.shape[1] // E
    group_size = HQ // KV
    kv_count = max(head_local // group_size, 1)
    per_kv = head_local // kv_count
    tp_index = lax.axis_index("tp")
    sp_index = lax.axis_index("sp")
    sp_n = lax.axis_size("sp")
    tp_n = lax.axis_size("tp")
    columns = residual.shape[1]
    square = tp_n == 4
    half = columns // 2

    def sp_swap(x, s):
        return lax.ppermute(x, "sp", [(i, i ^ s) for i in range(sp_n)])

    def tp_swap(x, s):
        return lax.ppermute(x, "tp", [(i, i ^ s) for i in range(tp_n)])

    if square:
        offs = jnp.stack(
            [(tp_index ^ s) * columns + h * half for s in range(4) for h in range(2)]
        ).astype(jnp.int32)
        blocks = [(2, 6), (5, 7), (0, 4), (1, 3)]
        width = half
    else:
        offs = jnp.zeros((1,), jnp.int32)
        blocks = [(0,)]
        width = D

    def scatter_sum(parts):
        if not square:
            return lax.psum_scatter(parts[0], "tp", scatter_dimension=1, tiled=True).astype(f32)
        far_a, far_b, near_a, near_b = parts
        sum_a = near_a.astype(f32) + tp_swap(far_a, 1).astype(f32)
        sum_b = near_b.astype(f32) + tp_swap(far_b, 2).astype(f32)
        last_a = tp_swap(sum_a[:, half:].astype(bf16), 2)
        last_b = tp_swap(sum_b[:, half:].astype(bf16), 1)
        return jnp.concatenate(
            [sum_a[:, :half] + last_a.astype(f32), sum_b[:, :half] + last_b.astype(f32)], axis=1
        )

    kv_first = tp_index * head_local // group_size
    positions = sp_index * tok_rows + jnp.arange(tok_rows, dtype=jnp.int32)
    key_cols = lax.dynamic_slice_in_dim(key_heads, kv_first * E, kv_count * E, 1)
    value_cols = lax.dynamic_slice_in_dim(value_heads, kv_first * E, kv_count * E, 1)
    k_turned = turn(key_cols.astype(f32), k_gain, kv_count, positions)
    kv_own = jnp.concatenate(
        [
            part[:, c * E : (c + 1) * E]
            for c in range(kv_count)
            for part in (k_turned, value_cols)
        ],
        axis=1,
    )
    firsts = [kv_own] + [sp_swap(kv_own, s) for s in range(2, sp_n, 2)]
    firsts = jnp.concatenate(firsts, axis=0)
    kv_pieces = [firsts, sp_swap(firsts, 1)]
    q_turned = turn(query_heads.astype(f32), q_gain, head_local, positions)
    q_wide = jnp.concatenate(
        [q_turned.reshape(tok_rows, head_local, E), jnp.zeros((tok_rows, head_local, E), bf16)],
        axis=2,
    ).reshape(tok_rows, head_local * 2 * E)

    capacity = 5 * tok_rows * TOPK // (4 * sp_n) + 1
    slots = -(-capacity // 8) * 8
    order = sp_index ^ jnp.arange(sp_n, dtype=jnp.int32)
    named = (routes[:, :, None] == order[None, None, :]).astype(f32)
    counts = jnp.sum(named, axis=1)
    below = (
        jnp.arange(tok_rows)[:, None] > jnp.arange(tok_rows)[None, :]
    ).astype(bf16)
    before = jnp.dot(below, counts.astype(bf16), preferred_element_type=f32)
    slot_at = jnp.where(counts > 0, before, -1.0)
    pick = (
        slot_at.T[:, None, :] == jnp.arange(slots, dtype=f32)[None, :, None]
    ).astype(bf16).reshape(sp_n * slots, tok_rows)
    slot_of_k = jnp.sum(
        named * (before + jnp.arange(sp_n, dtype=f32)[None, :] * slots)[:, None, :], axis=2
    )
    take = [
        (slot_of_k[:, k : k + 1] == jnp.arange(sp_n * slots, dtype=f32)[None, :]).astype(bf16)
        for k in range(TOPK)
    ]

    if square:
        gain_parts = [norm_gain] + [tp_swap(norm_gain, s) for s in (1, 2, 3)]
        gain_all = jnp.zeros((D,), f32)
        for s in range(4):
            gain_all = lax.dynamic_update_slice(
                gain_all, gain_parts[s], ((tp_index ^ s) * columns,)
            )
    else:
        gain_all = lax.all_gather(norm_gain, "tp", axis=0, tiled=True)
    gain_all = gain_all[None, :]

    vmem = pl.BlockSpec(memory_space=pltpu.VMEM)
    smem = pl.BlockSpec(memory_space=pltpu.SMEM)
    part_shapes = lambda rows: [
        jax.ShapeDtypeStruct((rows, width * len(indices)), bf16) for indices in blocks
    ]
    parts = pl.pallas_call(
        attention_kernel(blocks, width, kv_count, per_kv, len(kv_pieces)),
        out_shape=part_shapes(tok_rows),
        in_specs=[smem] + [vmem] * (2 + len(kv_pieces)),
        out_specs=[vmem] * len(blocks),
        scratch_shapes=[
            pltpu.VMEM((sp_n * tok_rows, kv_count * 2 * E), bf16),
            pltpu.VMEM((tok_rows, head_local * E), bf16),
            pltpu.VMEM((tok_rows, D), f32),
        ],
        compiler_params=pltpu.CompilerParams(vmem_limit_bytes=56 * 1024 * 1024),
        name="attention",
    )(offs, q_wide, *kv_pieces, out_weight)
    after_attn = residual.astype(f32) + scatter_sum(parts)
    scaled = (after_attn * norm_gain[None, :]).astype(bf16)

    sent = jnp.dot(pick, scaled, preferred_element_type=f32).astype(bf16)
    per_group = sp_n // GROUPS
    hidden = w_gate.shape[2]
    hidden_block = min(hidden, 256)
    steps = hidden // hidden_block
    picked = [None] * TOPK
    for group in range(GROUPS):
        arrived = []
        for s in range(group * per_group, (group + 1) * per_group):
            piece = sent[s * slots : (s + 1) * slots]
            arrived.append(sp_swap(piece, s) if s else piece)
        own = jnp.concatenate(arrived, axis=0)
        rows = own.shape[0]
        if square:
            side_x = tp_swap(own, 1)
            side_y = tp_swap(own, 2)
            inputs = [own, side_x, side_y, tp_swap(side_y[:, :half], 1), tp_swap(side_x[:, half:], 2)]
            in_offs = (0, 2, 4, 6, 7)
        else:
            inputs = [lax.all_gather(own, "tp", axis=1, tiled=True)]
            in_offs = (0,)
        whole = lambda x: pl.BlockSpec(x.shape, lambda f: (0, 0))
        parts = pl.pallas_call(
            expert_kernel(blocks, width, in_offs, len(inputs), steps),
            grid=(steps,),
            out_shape=part_shapes(rows),
            in_specs=[smem, whole(gain_all)]
            + [whole(x) for x in inputs]
            + [
                pl.BlockSpec((1, D, hidden_block), lambda f: (0, 0, f)),
                pl.BlockSpec((1, D, hidden_block), lambda f: (0, 0, f)),
                pl.BlockSpec((1, hidden_block, D), lambda f: (0, f, 0)),
            ],
            out_specs=[
                pl.BlockSpec((rows, width * len(indices)), lambda f: (0, 0)) for indices in blocks
            ],
            scratch_shapes=[pltpu.VMEM((rows, D), f32), pltpu.VMEM((rows, 128), f32)],
            compiler_params=pltpu.CompilerParams(vmem_limit_bytes=40 * 1024 * 1024),
            name="experts",
        )(offs, gain_all, *inputs, w_gate, w_up, w_down)
        expert_rows = scatter_sum(parts).astype(bf16)
        returned = []
        for n in range(per_group):
            s = group * per_group + n
            piece = expert_rows[n * slots : (n + 1) * slots]
            returned.append(sp_swap(piece, s) if s else piece)
        returned = jnp.concatenate(returned, axis=0)
        for k in range(TOPK):
            part = jnp.dot(
                take[k][:, group * per_group * slots : (group + 1) * per_group * slots],
                returned,
                preferred_element_type=f32,
            )
            picked[k] = part if picked[k] is None else picked[k] + part
    expert_mix = picked[0] * route_weights[:, 0:1]
    for k in range(1, TOPK):
        expert_mix = expert_mix + picked[k] * route_weights[:, k : k + 1]
    return (after_attn + expert_mix).astype(bf16)


def solution(mesh):
    return jax.shard_map(
        shards,
        mesh=mesh,
        in_specs=(
            P("sp", "tp"),
            P("sp", None),
            P("sp", None),
            P(),
            P(),
            P("tp", None),
            P("sp", "tp"),
            P("tp"),
            P("sp", None),
            P("sp", None),
            P("sp", None, "tp"),
            P("sp", None, "tp"),
            P("sp", "tp", None),
        ),
        out_specs=P("sp", "tp"),
        check_vma=False,
    )
```

```python
import jax
import jax.numpy as jnp
from jax import lax
from jax.experimental import pallas as pl
from jax.experimental.pallas import tpu as pltpu
from jax.sharding import PartitionSpec as P

D = 2048
HQ = 16
KV = 4
E = 64
TOPK = 2
GRID_W = 64
GROUPS = 4

norm_eps = 1e-06
rope_base = 10000.0
bf16 = jnp.bfloat16
f32 = jnp.float32


def turn(values, gain, heads, positions):
    rows, width = values.shape
    lane = jnp.arange(width, dtype=jnp.int32) % E
    quarter = E // 4
    same_head = (jnp.arange(width)[:, None] // E == jnp.arange(heads)[None, :]).astype(f32)
    mean_sq = jnp.dot(values * values, same_head, precision=lax.Precision.HIGHEST) / E
    scale = jnp.dot(
        lax.rsqrt(mean_sq + norm_eps), same_head.T, precision=lax.Precision.HIGHEST
    )
    normed = values * scale * jnp.tile(gain, heads)[None, :]
    frequency = rope_base ** (-jnp.arange(quarter, dtype=f32) / quarter)
    grid_rows = (positions // GRID_W).astype(f32)
    grid_cols = (positions % GRID_W).astype(f32)
    angles = jnp.concatenate(
        [grid_rows[:, None] * frequency[None, :], grid_cols[:, None] * frequency[None, :]], axis=1
    )
    cosine = jnp.cos(angles)
    sines = jnp.sin(angles)
    cos_lane = jnp.concatenate([cosine[:, :quarter]] * 2 + [cosine[:, quarter:]] * 2, axis=1)
    sin_lane = jnp.concatenate(
        [-sines[:, :quarter], sines[:, :quarter], -sines[:, quarter:], sines[:, quarter:]], axis=1
    )
    first = (lane % (2 * quarter)) < quarter
    other = jnp.where(
        first[None, :], jnp.roll(normed, -quarter, axis=1), jnp.roll(normed, quarter, axis=1)
    )
    return (
        normed * jnp.tile(cos_lane, (1, heads)) + other * jnp.tile(sin_lane, (1, heads))
    ).astype(bf16)


def write_parts(value, offs_ref, outs, blocks, width):
    for ref, indices in zip(outs, blocks):
        for place, index in enumerate(indices):
            start = offs_ref[index]
            if width < D:
                start = pl.multiple_of(start, 128)
                ref[:, place * width : (place + 1) * width] = value[:, pl.ds(start, width)].astype(
                    bf16
                )
            else:
                ref[...] = value[...].astype(bf16)


def attention_kernel(blocks, width, kv_count, per_kv, pieces):
    def body(offs_ref, q_ref, *refs):
        kv_refs = refs[:pieces]
        weight_ref = refs[pieces]
        outs = refs[pieces + 1 : pieces + 1 + len(blocks)]
        kv_all, attended, acc = refs[pieces + 1 + len(blocks) :]
        rows = kv_refs[0].shape[0]
        for n in range(pieces):
            kv_all[n * rows : (n + 1) * rows, :] = kv_refs[n][...]
        for c in range(kv_count):
            kv = kv_all[:, c * 2 * E : (c + 1) * 2 * E]
            for g in range(per_kv):
                h = c * per_kv + g
                q = q_ref[:, h * 2 * E : (h + 1) * 2 * E]
                scores = lax.dot_general(
                    q, kv, (((1,), (1,)), ((), ())), preferred_element_type=f32
                )
                scores = scores * (E**-0.5)
                exped = jnp.exp(scores - jnp.max(scores, axis=1, keepdims=True))
                total = jnp.sum(exped, axis=1, keepdims=True)
                mixed = jnp.dot(exped.astype(bf16), kv, preferred_element_type=f32)
                attended[:, h * E : (h + 1) * E] = (mixed[:, E:] / total).astype(bf16)
        acc[...] = jnp.dot(attended[...], weight_ref[...], preferred_element_type=f32)
        write_parts(acc, offs_ref, outs, blocks, width)

    return body


def expert_kernel(blocks, width, in_offs, pieces, steps):
    def body(offs_ref, gain_ref, *refs):
        u_refs = refs[:pieces]
        gate_ref, up_ref, down_ref = refs[pieces : pieces + 3]
        outs = refs[pieces + 3 : pieces + 3 + len(blocks)]
        acc, scale = refs[pieces + 3 + len(blocks) :]
        step = pl.program_id(0)

        @pl.when(step == 0)
        def _():
            total = None
            for n in range(pieces):
                wide = u_refs[n].shape[1]
                start = pl.multiple_of(offs_ref[in_offs[n]], 128)
                plain = u_refs[n][...].astype(f32) / gain_ref[:, pl.ds(start, wide)]
                part = jnp.sum(plain * plain, axis=1, keepdims=True)
                total = part if total is None else total + part
            scale[...] = jnp.broadcast_to(lax.rsqrt(total / D + norm_eps), scale.shape)

        gate = None
        up = None
        for n in range(pieces):
            wide = u_refs[n].shape[1]
            start = pl.multiple_of(offs_ref[in_offs[n]], 128)
            u = u_refs[n][...]
            g = jnp.dot(u, gate_ref[0, pl.ds(start, wide), :], preferred_element_type=f32)
            v = jnp.dot(u, up_ref[0, pl.ds(start, wide), :], preferred_element_type=f32)
            gate = g if gate is None else gate + g
            up = v if up is None else up + v
        factor = scale[:, 0:1]
        gate = gate * factor
        up = up * factor
        act = (gate / (1.0 + jnp.exp(-gate)) * up).astype(bf16)
        part = jnp.dot(act, down_ref[0], preferred_element_type=f32)

        @pl.when(step == 0)
        def _():
            acc[...] = part

        @pl.when(step > 0)
        def _():
            acc[...] += part

        @pl.when(step == steps - 1)
        def _():
            write_parts(acc, offs_ref, outs, blocks, width)

    return body


def shards(
    query_heads,
    key_heads,
    value_heads,
    q_gain,
    k_gain,
    out_weight,
    residual,
    norm_gain,
    routes,
    route_weights,
    w_gate,
    w_up,
    w_down,
):
    tok_rows = query_heads.shape[0]
    head_local = query_heads.shape[1] // E
    group_size = HQ // KV
    kv_count = max(head_local // group_size, 1)
    per_kv = head_local // kv_count
    tp_index = lax.axis_index("tp")
    sp_index = lax.axis_index("sp")
    sp_n = lax.axis_size("sp")
    tp_n = lax.axis_size("tp")
    columns = residual.shape[1]
    square = tp_n == 4
    half = columns // 2

    def sp_swap(x, s):
        return lax.ppermute(x, "sp", [(i, i ^ s) for i in range(sp_n)])

    def tp_swap(x, s):
        return lax.ppermute(x, "tp", [(i, i ^ s) for i in range(tp_n)])

    if square:
        offs = jnp.stack(
            [(tp_index ^ s) * columns + h * half for s in range(4) for h in range(2)]
        ).astype(jnp.int32)
        blocks = [(2, 6), (5, 7), (0, 4), (1, 3)]
        width = half
    else:
        offs = jnp.zeros((1,), jnp.int32)
        blocks = [(0,)]
        width = D

    def scatter_sum(parts):
        if not square:
            return lax.psum_scatter(parts[0], "tp", scatter_dimension=1, tiled=True).astype(f32)
        far_a, far_b, near_a, near_b = parts
        sum_a = near_a.astype(f32) + tp_swap(far_a, 1).astype(f32)
        sum_b = near_b.astype(f32) + tp_swap(far_b, 2).astype(f32)
        last_a = tp_swap(sum_a[:, half:].astype(bf16), 2)
        last_b = tp_swap(sum_b[:, half:].astype(bf16), 1)
        return jnp.concatenate(
            [sum_a[:, :half] + last_a.astype(f32), sum_b[:, :half] + last_b.astype(f32)], axis=1
        )

    kv_first = tp_index * head_local // group_size
    positions = sp_index * tok_rows + jnp.arange(tok_rows, dtype=jnp.int32)
    key_cols = lax.dynamic_slice_in_dim(key_heads, kv_first * E, kv_count * E, 1)
    value_cols = lax.dynamic_slice_in_dim(value_heads, kv_first * E, kv_count * E, 1)
    k_turned = turn(key_cols.astype(f32), k_gain, kv_count, positions)
    kv_own = jnp.concatenate(
        [
            part[:, c * E : (c + 1) * E]
            for c in range(kv_count)
            for part in (k_turned, value_cols)
        ],
        axis=1,
    )
    firsts = [kv_own] + [sp_swap(kv_own, s) for s in range(2, sp_n, 2)]
    firsts = jnp.concatenate(firsts, axis=0)
    kv_pieces = [firsts, sp_swap(firsts, 1)]
    q_turned = turn(query_heads.astype(f32), q_gain, head_local, positions)
    q_wide = jnp.concatenate(
        [q_turned.reshape(tok_rows, head_local, E), jnp.zeros((tok_rows, head_local, E), bf16)],
        axis=2,
    ).reshape(tok_rows, head_local * 2 * E)

    capacity = 5 * tok_rows * TOPK // (4 * sp_n) + 1
    slots = -(-capacity // 8) * 8
    order = sp_index ^ jnp.arange(sp_n, dtype=jnp.int32)
    named = (routes[:, :, None] == order[None, None, :]).astype(f32)
    counts = jnp.sum(named, axis=1)
    below = (
        jnp.arange(tok_rows)[:, None] > jnp.arange(tok_rows)[None, :]
    ).astype(bf16)
    before = jnp.dot(below, counts.astype(bf16), preferred_element_type=f32)
    slot_at = jnp.where(counts > 0, before, -1.0)
    pick = (
        slot_at.T[:, None, :] == jnp.arange(slots, dtype=f32)[None, :, None]
    ).astype(bf16).reshape(sp_n * slots, tok_rows)
    slot_of_k = jnp.sum(
        named * (before + jnp.arange(sp_n, dtype=f32)[None, :] * slots)[:, None, :], axis=2
    )
    take = [
        (slot_of_k[:, k : k + 1] == jnp.arange(sp_n * slots, dtype=f32)[None, :]).astype(bf16)
        for k in range(TOPK)
    ]

    if square:
        gain_parts = [norm_gain] + [tp_swap(norm_gain, s) for s in (1, 2, 3)]
        gain_all = jnp.zeros((D,), f32)
        for s in range(4):
            gain_all = lax.dynamic_update_slice(
                gain_all, gain_parts[s], ((tp_index ^ s) * columns,)
            )
    else:
        gain_all = lax.all_gather(norm_gain, "tp", axis=0, tiled=True)
    gain_all = gain_all[None, :]

    vmem = pl.BlockSpec(memory_space=pltpu.VMEM)
    smem = pl.BlockSpec(memory_space=pltpu.SMEM)
    part_shapes = lambda rows: [
        jax.ShapeDtypeStruct((rows, width * len(indices)), bf16) for indices in blocks
    ]
    parts = pl.pallas_call(
        attention_kernel(blocks, width, kv_count, per_kv, len(kv_pieces)),
        out_shape=part_shapes(tok_rows),
        in_specs=[smem] + [vmem] * (2 + len(kv_pieces)),
        out_specs=[vmem] * len(blocks),
        scratch_shapes=[
            pltpu.VMEM((sp_n * tok_rows, kv_count * 2 * E), bf16),
            pltpu.VMEM((tok_rows, head_local * E), bf16),
            pltpu.VMEM((tok_rows, D), f32),
        ],
        compiler_params=pltpu.CompilerParams(vmem_limit_bytes=56 * 1024 * 1024),
        name="attention",
    )(offs, q_wide, *kv_pieces, out_weight)
    after_attn = residual.astype(f32) + scatter_sum(parts)
    scaled = (after_attn * norm_gain[None, :]).astype(bf16)

    sent = jnp.dot(pick, scaled, preferred_element_type=f32).astype(bf16)
    chips = sp_n // 2
    per_group = chips // GROUPS
    hidden = w_gate.shape[2]
    hidden_block = min(hidden, 512)
    steps = hidden // hidden_block
    picked = [None] * TOPK
    for group in range(GROUPS):
        crossed = []
        for k in range(group * per_group, (group + 1) * per_group):
            pair = sent[2 * k * slots : (2 * k + 2) * slots]
            crossed.append(sp_swap(pair, 2 * k) if k else pair)
        for_other = jnp.concatenate([pair[slots:] for pair in crossed], axis=0)
        own = jnp.concatenate(
            [pair[:slots] for pair in crossed] + [sp_swap(for_other, 1)], axis=0
        )
        rows = own.shape[0]
        if square:
            side_x = tp_swap(own, 1)
            side_y = tp_swap(own, 2)
            inputs = [own, side_x, side_y, tp_swap(side_y[:, :half], 1), tp_swap(side_x[:, half:], 2)]
            in_offs = (0, 2, 4, 6, 7)
        else:
            inputs = [lax.all_gather(own, "tp", axis=1, tiled=True)]
            in_offs = (0,)
        whole = lambda x: pl.BlockSpec(x.shape, lambda f: (0, 0))
        parts = pl.pallas_call(
            expert_kernel(blocks, width, in_offs, len(inputs), steps),
            grid=(steps,),
            out_shape=part_shapes(rows),
            in_specs=[smem, whole(gain_all)]
            + [whole(x) for x in inputs]
            + [
                pl.BlockSpec((1, D, hidden_block), lambda f: (0, 0, f)),
                pl.BlockSpec((1, D, hidden_block), lambda f: (0, 0, f)),
                pl.BlockSpec((1, hidden_block, D), lambda f: (0, f, 0)),
            ],
            out_specs=[
                pl.BlockSpec((rows, width * len(indices)), lambda f: (0, 0)) for indices in blocks
            ],
            scratch_shapes=[pltpu.VMEM((rows, D), f32), pltpu.VMEM((rows, 128), f32)],
            compiler_params=pltpu.CompilerParams(vmem_limit_bytes=40 * 1024 * 1024),
            name="experts",
        )(offs, gain_all, *inputs, w_gate, w_up, w_down)
        expert_rows = scatter_sum(parts).astype(bf16)
        middle = per_group * slots
        from_other = sp_swap(expert_rows[middle:], 1)
        returned = []
        for n in range(per_group):
            k = group * per_group + n
            pair = jnp.concatenate(
                [
                    expert_rows[n * slots : (n + 1) * slots],
                    from_other[n * slots : (n + 1) * slots],
                ],
                axis=0,
            )
            returned.append(sp_swap(pair, 2 * k) if k else pair)
        returned = jnp.concatenate(returned, axis=0)
        for k in range(TOPK):
            part = jnp.dot(
                take[k][:, 2 * group * middle : 2 * (group + 1) * middle],
                returned,
                preferred_element_type=f32,
            )
            picked[k] = part if picked[k] is None else picked[k] + part
    expert_mix = picked[0] * route_weights[:, 0:1]
    for k in range(1, TOPK):
        expert_mix = expert_mix + picked[k] * route_weights[:, k : k + 1]
    return (after_attn + expert_mix).astype(bf16)


def solution(mesh):
    return jax.shard_map(
        shards,
        mesh=mesh,
        in_specs=(
            P("sp", "tp"),
            P("sp", None),
            P("sp", None),
            P(),
            P(),
            P("tp", None),
            P("sp", "tp"),
            P("tp"),
            P("sp", None),
            P("sp", None),
            P("sp", None, "tp"),
            P("sp", None, "tp"),
            P("sp", "tp", None),
        ),
        out_specs=P("sp", "tp"),
        check_vma=False,
    )
```
